32 devices in a mesh: fs: 4 (over y, x), tp: 8 (over z, core).
Axes of the slice: x: 2, y: 2, z: 4, core: 2. Of those that a mesh axis runs over, the one named last changes fastest.
Arguments:
- tokens_in: bfloat16 [8192, 2048], P(('fs', 'tp')), may hold values from -6 to 6
- gate_cotangent: bfloat16 [8192, 1024], P(('fs', 'tp')), may hold values from -0.125 to 0.125
- conv_output: bfloat16 [8192, 1024], P(('fs', 'tp')), may hold values from -6 to 6
- block_cotangent: bfloat16 [8192, 2048], P(('fs', 'tp')), may hold values from -0.125 to 0.125
- projectors: bfloat16 [2048, 2, 256], P('fs'), may hold values from -0.125 to 0.125
- first_moment: float32 [256, 2, 1024], P('fs', None, 'tp'), may hold values from -6 to 6
- second_moment: float32 [256, 2, 1024], P('fs', None, 'tp'), may hold values from 0.25 to 4
- gate_master: float32 [2048, 1024], P('fs', 'tp'), may hold values from -0.125 to 0.125
- out_master: float32 [1024, 2048], P('tp', 'fs'), may hold values from -0.1875 to 0.1875
Outputs:
- first_new: float32 [256, 2, 1024], P('fs', None, 'tp')
- second_new: float32 [256, 2, 1024], P('fs', None, 'tp')
- step_gate: float32 [2048, 1024], P('fs', 'tp')
- step_out: float32 [1024, 2048], P('tp', 'fs')
- gate_new: float32 [2048, 1024], P('fs', 'tp')
- out_new: float32 [1024, 2048], P('tp', 'fs')
- gate_copy: bfloat16 [2048, 1024], P(None, 'tp')
- out_copy: bfloat16 [1024, 2048], P('tp')
The draws below stay inside these ranges and needn't reach their ends.
All inputs are finite; a program needn't handle non-finite values.
Results may differ from the reference program's by a relative error of at most 0.0035.
Values may be sent and summed in bfloat16 or wider, within the bound.
A program may use at most 64 MiB of HBM per device.

```python
import math
import jax
import jax.numpy as jnp
from jax import lax

D = 2048
CH = 1024
RANK = 256
TOKENS = 8192


def raised(result, rng, source, target, parts, factor):
    owner, partner = [(jnp.arange(result.shape[dim]) // (result.shape[dim] // parts)).reshape([-1 if axis == dim else 1 for axis in range(result.ndim)]) for dim in (source, target)]
    chosen = jax.random.permutation(rng, parts)[partner]
    strong = (owner == chosen) | (owner == (partner + parts // 2) % parts)
    return jnp.where(strong, factor * result, result)


def block_scale(own_key, shape, cuts, least, top_value):
    factor_of = 1.0
    for position, shards_of in cuts:
        steps = jax.random.uniform(jax.random.fold_in(jax.random.fold_in(own_key, 6), position), (shards_of,), jnp.float32, least / len(cuts), top_value / len(cuts))
        factor_of = factor_of * jnp.repeat(jnp.exp(steps), shape[position] // shards_of).reshape((-1,) + (1,) * (len(shape) - 1 - position))
    return factor_of


def scatter_about(stream_key, shape, deviation, bound, pieces=(), held_as=jnp.bfloat16):
    entries = jax.random.normal(stream_key, shape, jnp.float32) * deviation
    if len(pieces) > 0:
        entries = block_scale(stream_key, shape, pieces, -0.22, 0.18) * entries
    return jnp.clip(entries, min=-bound, max=bound).astype(held_as)


def heavy_noise(rng, shape, width, reach, pieces, heavy, held_as=jnp.bfloat16):
    result = width * jax.random.normal(rng, shape, jnp.float32)
    if pieces:
        result = result * block_scale(rng, shape, pieces, -0.22, 0.18)
    return jnp.clip(raised(result, jax.random.fold_in(rng, 3), *heavy), -reach, reach).astype(held_as)


def setup_inputs(seed: int = 0) -> dict:
    keys = jax.random.split(jax.random.key(seed), 10)
    return {
        "tokens_in": scatter_about(keys[0], (TOKENS, D), 1.0, 6.0, ((0, 32),)),
        "gate_cotangent": heavy_noise(keys[1], (TOKENS, CH), (TOKENS ** -0.5), 0.125, ((0, 32),), (0, 1, 32, 2.75)),
        "conv_output": scatter_about(keys[2], (TOKENS, CH), 1.0, 6.0, ((0, 32),)),
        "block_cotangent": heavy_noise(keys[3], (TOKENS, D), (TOKENS ** -0.5), 0.125, ((0, 32),), (0, 1, 32, 2.75)),
        "projectors": scatter_about(keys[4], (D, 2, RANK), D ** -0.5, 0.125, ((0, 4),)),
        "first_moment": scatter_about(keys[5], (RANK, 2, CH), 1.0, 6.0, ((0, 4), (2, 8)), jnp.float32),
        "second_moment": jnp.clip(jnp.exp(math.log(4.0) - 2.7725887 * jax.random.uniform(keys[6], (RANK, 2, CH), jnp.float32) ** block_scale(keys[6], (RANK, 2, CH), ((0, 4), (2, 8)), -0.2, 0.2)), 0.25, 4.0),
        "gate_master": scatter_about(keys[7], (D, CH), D ** -0.5, 0.125, ((0, 4), (1, 8)), jnp.float32),
        "out_master": scatter_about(keys[8], (CH, D), CH ** -0.5, 0.1875, ((0, 8), (1, 4)), jnp.float32),
    }


def reference(tokens_in, gate_cotangent, conv_output, block_cotangent, projectors, first_moment, second_moment, gate_master, out_master):
    contract_dims = (((0,), (0,)), ((), ()))
    grad_gate = lax.dot_general(tokens_in, gate_cotangent, contract_dims, preferred_element_type=jnp.float32)
    grad_flip = lax.dot_general(block_cotangent, conv_output, contract_dims, preferred_element_type=jnp.float32)
    gradients = jnp.stack((grad_gate, grad_flip), axis=1)
    proj_wide = projectors.astype(jnp.float32)
    low_space = jnp.einsum('dmr,dmc->rmc', proj_wide, gradients, precision=lax.Precision.HIGHEST)
    first_new = 0.8 * first_moment + 0.2 * low_space
    second_new = 0.9 * second_moment + 0.1 * low_space * low_space
    direction = first_new / jnp.sqrt(second_new)
    norm_value = jnp.sqrt(lax.optimization_barrier(jnp.sum(direction * direction, axis=(0, 2))))
    clip_level = 0.5 * math.sqrt(RANK * CH)
    factor = clip_level / jnp.maximum(norm_value, clip_level)
    scaled_step = jnp.einsum('dmr,rmc->dmc', proj_wide, direction, precision=lax.Precision.HIGHEST) * factor[None, :, None]
    step_gate = scaled_step[:, 0, :]
    step_out = scaled_step[:, 1, :].T
    gate_new = gate_master - 0.01 * step_gate
    out_new = out_master - 0.01 * step_out
    return (first_new, second_new, step_gate, step_out, gate_new, out_new, gate_new.astype(jnp.bfloat16), out_new.astype(jnp.bfloat16))
```

```python
import functools
import math

import jax
import jax.numpy as jnp
from jax import lax
from jax.experimental import pallas as pl
from jax.experimental.pallas import tpu as pltpu
from jax.sharding import PartitionSpec as P

BETA_FIRST = 0.8
BETA_SECOND = 0.9
LEARN_RATE = 0.01
CLIP_SHARE = 0.5
MESH_ID = pl.DeviceIdType.MESH
WIDE = jnp.float32
SLIM = jnp.bfloat16


def update_kernel(
    fs_total,
    tp_total,
    clip_level,
    tokens_in,
    gate_cot,
    conv_out,
    block_cot,
    proj,
    first_old,
    second_old,
    gate_old,
    out_old,
    first_new,
    second_new,
    step_gate,
    step_out,
    gate_new,
    out_new,
    gate_copy,
    out_copy,
    left,
    right,
    peers_proj,
    mix,
    low,
    fs_out,
    fs_in,
    tile_sum,
    tp_out,
    tp_in,
    dirs,
    squares,
    swap_send,
    swap_recv,
    load_sem,
    proj_send,
    proj_recv,
    fs_send,
    fs_recv,
    tp_send,
    tp_recv,
    dir_send,
    dir_recv,
    square_send,
    square_recv,
    gate_send,
    gate_recv,
    out_send,
    out_recv,
):
    me_fs = lax.axis_index("fs")
    me_tp = lax.axis_index("tp")
    core = lax.rem(me_tp, 2)
    partner = me_tp + 1 - 2 * core
    rows_d, rank = proj.shape[1], proj.shape[2]
    rank_rows = rank // fs_total
    width = gate_old.shape[1]
    local = tokens_in.shape[0]

    def fs_peer(step):
        return lax.rem(me_fs + step, fs_total)

    def fs_source(step):
        return lax.rem(me_fs + fs_total - step, fs_total)

    def tp_peer(step):
        return lax.rem(me_tp + step, tp_total)

    def send_fs(source, target, send_sem, recv_sem, step):
        return pltpu.make_async_remote_copy(
            src_ref=source,
            dst_ref=target,
            send_sem=send_sem.at[step],
            recv_sem=recv_sem.at[step],
            device_id={"fs": fs_peer(step), "tp": me_tp},
            device_id_type=MESH_ID,
        )

    def send_tp(source, target, send_sem, recv_sem, step, target_tp):
        return pltpu.make_async_remote_copy(
            src_ref=source,
            dst_ref=target,
            send_sem=send_sem.at[step],
            recv_sem=recv_sem.at[step],
            device_id={"fs": me_fs, "tp": target_tp},
            device_id_type=MESH_ID,
        )

    def own_copy(source, target, slot):
        return pltpu.make_async_copy(source, target, load_sem.at[slot])

    @pl.when(core == 0)
    def _():
        own_copy(tokens_in, left.at[0], 0).start()
        own_copy(gate_cot, right.at[0], 1).start()

    @pl.when(core == 1)
    def _():
        own_copy(block_cot, left.at[0], 0).start()
        own_copy(conv_out, right.at[0], 1).start()

    barrier = pltpu.get_barrier_semaphore()
    for step in range(1, fs_total):
        pl.semaphore_signal(
            barrier, inc=1, device_id={"fs": fs_peer(step), "tp": me_tp}, device_id_type=MESH_ID
        )
    for step in range(1, tp_total):
        pl.semaphore_signal(
            barrier, inc=1, device_id={"fs": me_fs, "tp": tp_peer(step)}, device_id_type=MESH_ID
        )
    pl.semaphore_wait(barrier, fs_total + tp_total - 2)

    proj_copies = [None]
    for step in range(1, fs_total):
        copy = send_fs(proj.at[core], peers_proj.at[step], proj_send, proj_recv, step)
        copy.start()
        proj_copies.append(copy)

    swap_left = send_tp(block_cot, left.at[1], swap_send, swap_recv, 0, partner)
    swap_right = send_tp(conv_out, right.at[1], swap_send, swap_recv, 1, partner)

    @pl.when(core == 0)
    def _():
        swap_left.start()
        swap_right.start()

    @pl.when(core == 1)
    def _():
        send_tp(tokens_in, left.at[1], swap_send, swap_recv, 0, partner).start()
        send_tp(gate_cot, right.at[1], swap_send, swap_recv, 1, partner).start()

    own_copy(tokens_in, left.at[0], 0).wait()
    swap_left.wait_recv()

    def mixed(block, factor_rows):
        columns = pl.ds(pl.multiple_of(block * rows_d, 128), rows_d)
        part = left[:, :, columns].reshape(2 * local, rows_d)
        return jnp.dot(part, factor_rows, preferred_element_type=WIDE)

    mix[...] = mixed(me_fs, proj[core])
    for step in range(1, fs_total):
        proj_copies[step].wait_recv()
        mix[...] += mixed(fs_source(step), peers_proj[step])

    own_copy(gate_cot, right.at[0], 1).wait()
    swap_right.wait_recv()
    upper = mix[...].astype(SLIM)
    lower = (mix[...] - upper.astype(WIDE)).astype(SLIM)
    cots = right[...].reshape(2 * local, right.shape[2])
    dims = (((0,), (0,)), ((), ()))
    low[...] = lax.dot_general(upper, cots, dims, preferred_element_type=WIDE) + lax.dot_general(
        lower, cots, dims, preferred_element_type=WIDE
    )

    def low_rows(block):
        return low[pl.ds(pl.multiple_of(block * rank_rows, 8), rank_rows), :]

    fs_copies = [None]
    for step in range(1, fs_total):
        rows = low_rows(fs_peer(step)).astype(SLIM)
        for tile in range(tp_total):
            fs_out[step, tile] = rows[:, tile * width : (tile + 1) * width]
        copy = send_fs(fs_out.at[step], fs_in.at[step], fs_send, fs_recv, step)
        copy.start()
        fs_copies.append(copy)
    rows = low_rows(me_fs)
    for tile in range(tp_total):
        tile_sum[tile] = rows[:, tile * width : (tile + 1) * width]
    for step in range(1, fs_total):
        fs_copies[step].wait_recv()
        tile_sum[...] += fs_in[step].astype(WIDE)

    tp_copies = [None]
    for step in range(1, tp_total):
        tp_out[step] = tile_sum[tp_peer(step)].astype(SLIM)
        copy = send_tp(tp_out.at[step], tp_in.at[step], tp_send, tp_recv, step, tp_peer(step))
        copy.start()
        tp_copies.append(copy)
    same = tile_sum[me_tp]
    other = None
    for step in range(1, tp_total):
        tp_copies[step].wait_recv()
        piece = tp_in[step].astype(WIDE)
        if step % 2 == 0:
            same = same + piece
        else:
            other = piece if other is None else other + piece

    lows = (jnp.where(core == 0, same, other), jnp.where(core == 0, other, same))
    for index in range(2):
        picked = pl.ds(index, rank_rows, stride=2)
        first = BETA_FIRST * first_old[picked, :] + (1.0 - BETA_FIRST) * lows[index]
        second = BETA_SECOND * second_old[picked, :] + (1.0 - BETA_SECOND) * lows[index] * lows[index]
        first_new[picked, :] = first
        second_new[picked, :] = second
        dirs[me_fs, index] = (first / jnp.sqrt(second)).astype(SLIM)

    dir_copies = [None]
    for step in range(1, fs_total):
        copy = send_fs(dirs.at[me_fs], dirs.at[me_fs], dir_send, dir_recv, step)
        copy.start()
        dir_copies.append(copy)
    for step in range(1, fs_total):
        dir_copies[step].wait_recv()

    gate_dir = dirs[:, 0].reshape(rank, width)
    flip_dir = dirs[:, 1].reshape(rank, width)
    gate_wide = gate_dir.astype(WIDE)
    flip_wide = flip_dir.astype(WIDE)
    squares[0, 0] = jnp.sum((gate_wide * gate_wide).reshape(rank // 8, 8, width), axis=0)
    squares[0, 1] = jnp.sum((flip_wide * flip_wide).reshape(rank // 8, 8, width), axis=0)
    square_copies = [None]
    for step in range(1, tp_total):
        copy = send_tp(
            squares.at[0], squares.at[step], square_send, square_recv, step, tp_peer(step)
        )
        copy.start()
        square_copies.append(copy)
    raw_gate = jnp.dot(proj[0], gate_dir, preferred_element_type=WIDE)
    raw_out = lax.dot_general(
        flip_dir, proj[1], (((0,), (1,)), ((), ())), preferred_element_type=WIDE
    )
    for step in range(1, tp_total):
        square_copies[step].wait_recv()
    totals = jnp.sum(squares[...], axis=0)
    gate_norm = jnp.sqrt(jnp.sum(totals[0], keepdims=True))
    flip_norm = jnp.sqrt(jnp.sum(totals[1], keepdims=True))
    scaled_gate = raw_gate * (clip_level / jnp.maximum(gate_norm, clip_level))
    scaled_out = raw_out * (clip_level / jnp.maximum(flip_norm, clip_level))
    step_gate[...] = scaled_gate
    step_out[...] = scaled_out
    fresh_gate = gate_old[...] - LEARN_RATE * scaled_gate
    fresh_out = out_old[...] - LEARN_RATE * scaled_out
    own_rows = pl.ds(pl.multiple_of(me_fs * rows_d, 128), rows_d)
    gate_copy[own_rows, :] = fresh_gate.astype(SLIM)
    out_copy[:, own_rows] = fresh_out.astype(SLIM)
    gate_block = gate_copy.at[own_rows, :]
    out_block = out_copy.at[:, own_rows]
    last_copies = []
    for step in range(1, fs_total):
        copy = send_fs(gate_block, gate_block, gate_send, gate_recv, step)
        copy.start()
        last_copies.append(copy)
        copy = send_fs(out_block, out_block, out_send, out_recv, step)
        copy.start()
        last_copies.append(copy)
    gate_new[...] = fresh_gate
    out_new[...] = fresh_out
    for step in range(1, fs_total):
        proj_copies[step].wait_send()
        fs_copies[step].wait_send()
        dir_copies[step].wait_send()
    for step in range(1, tp_total):
        tp_copies[step].wait_send()
        square_copies[step].wait_send()
    swap_left.wait_send()
    swap_right.wait_send()
    for copy in last_copies:
        copy.wait()


def shards(
    tokens_in,
    gate_cotangent,
    conv_output,
    block_cotangent,
    projectors,
    first_moment,
    second_moment,
    gate_master,
    out_master,
):
    fs_total = lax.axis_size("fs")
    tp_total = lax.axis_size("tp")
    local, model = tokens_in.shape
    channels = gate_cotangent.shape[1]
    rows_d, _, rank = projectors.shape
    rank_rows, _, width = first_moment.shape
    clip_level = CLIP_SHARE * math.sqrt(rank * channels)
    proj = jnp.transpose(projectors, (1, 0, 2))
    flat = (2 * rank_rows, width)
    shape = jax.ShapeDtypeStruct
    whole = pl.BlockSpec(memory_space=pltpu.VMEM)
    away = pl.BlockSpec(memory_space=pl.ANY)
    fs_sems = pltpu.SemaphoreType.DMA((fs_total,))
    tp_sems = pltpu.SemaphoreType.DMA((tp_total,))
    two_sems = pltpu.SemaphoreType.DMA((2,))
    results = pl.pallas_call(
        functools.partial(update_kernel, fs_total, tp_total, clip_level),
        out_shape=(
            shape(flat, WIDE),
            shape(flat, WIDE),
            shape((rows_d, width), WIDE),
            shape((width, rows_d), WIDE),
            shape((rows_d, width), WIDE),
            shape((width, rows_d), WIDE),
            shape((model, width), SLIM),
            shape((width, model), SLIM),
        ),
        in_specs=[away] * 4 + [whole] * 5,
        out_specs=(whole,) * 8,
        scratch_shapes=[
            pltpu.VMEM((2, local, model), SLIM),
            pltpu.VMEM((2, local, channels), SLIM),
            pltpu.VMEM((fs_total, rows_d, rank), SLIM),
            pltpu.VMEM((2 * local, rank), WIDE),
            pltpu.VMEM((rank, channels), WIDE),
            pltpu.VMEM((fs_total, tp_total, rank_rows, width), SLIM),
            pltpu.VMEM((fs_total, tp_total, rank_rows, width), SLIM),
            pltpu.VMEM((tp_total, rank_rows, width), WIDE),
            pltpu.VMEM((tp_total, rank_rows, width), SLIM),
            pltpu.VMEM((tp_total, rank_rows, width), SLIM),
            pltpu.VMEM((fs_total, 2, rank_rows, width), SLIM),
            pltpu.VMEM((tp_total, 2, 8, width), WIDE),
            two_sems,
            two_sems,
            two_sems,
            fs_sems,
            fs_sems,
            fs_sems,
            fs_sems,
            tp_sems,
            tp_sems,
            fs_sems,
            fs_sems,
            tp_sems,
            tp_sems,
            fs_sems,
            fs_sems,
            fs_sems,
            fs_sems,
        ],
        compiler_params=pltpu.CompilerParams(
            collective_id=0, has_side_effects=True, vmem_limit_bytes=40 * 1024 * 1024
        ),
    )(
        tokens_in,
        gate_cotangent,
        conv_output,
        block_cotangent,
        proj,
        first_moment.reshape(flat),
        second_moment.reshape(flat),
        gate_master,
        out_master,
    )
    first_new, second_new = (part.reshape(rank_rows, 2, width) for part in results[:2])
    return (first_new, second_new) + tuple(results[2:])


def solution(mesh):
    in_specs = (
        P(("fs", "tp"), None),
        P(("fs", "tp"), None),
        P(("fs", "tp"), None),
        P(("fs", "tp"), None),
        P("fs", None, None),
        P("fs", None, "tp"),
        P("fs", None, "tp"),
        P("fs", "tp"),
        P("tp", "fs"),
    )
    out_specs = (
        P("fs", None, "tp"),
        P("fs", None, "tp"),
        P("fs", "tp"),
        P("tp", "fs"),
        P("fs", "tp"),
        P("tp", "fs"),
        P(None, "tp"),
        P("tp", None),
    )
    return jax.shard_map(shards, mesh=mesh, in_specs=in_specs, out_specs=out_specs, check_vma=False)
```

```python
import functools
import math

import jax
import jax.numpy as jnp
from jax import lax
from jax.experimental import pallas as pl
from jax.experimental.pallas import tpu as pltpu
from jax.sharding import PartitionSpec as P

BETA_FIRST = 0.8
BETA_SECOND = 0.9
LEARN_RATE = 0.01
CLIP_SHARE = 0.5
MESH_ID = pl.DeviceIdType.MESH
WIDE = jnp.float32
SLIM = jnp.bfloat16


def exchange_kernel(
    fs_total,
    tp_total,
    tokens_in,
    gate_cot,
    conv_out,
    block_cot,
    proj,
    first_hbm,
    second_hbm,
    gate_hbm,
    out_hbm,
    first_new,
    second_new,
    dirs,
    squares,
    all_proj,
    gate_slim,
    out_slim,
    gate_old,
    out_old,
    left,
    right,
    mix,
    low,
    fs_out,
    fs_in,
    tile_sum,
    tp_out,
    tp_in,
    first_old,
    second_old,
    swap_send,
    swap_recv,
    load_sem,
    proj_send,
    proj_recv,
    pass_send,
    pass_recv,
    fs_send,
    fs_recv,
    tp_send,
    tp_recv,
    dir_send,
    dir_recv,
    square_send,
    square_recv,
    gate_send,
    gate_recv,
    out_send,
    out_recv,
):
    me_fs = lax.axis_index("fs")
    me_tp = lax.axis_index("tp")
    core = lax.rem(me_tp, 2)
    partner = me_tp + 1 - 2 * core
    rows_d, rank = proj.shape[1], proj.shape[2]
    rank_rows = rank // fs_total
    width = gate_old.shape[1]
    local = tokens_in.shape[0]

    def fs_peer(step):
        return lax.rem(me_fs + step, fs_total)

    def fs_source(step):
        return lax.rem(me_fs + fs_total - step, fs_total)

    def tp_peer(step):
        return lax.rem(me_tp + step, tp_total)

    def send_fs(source, target, send_sem, recv_sem, step):
        return pltpu.make_async_remote_copy(
            src_ref=source,
            dst_ref=target,
            send_sem=send_sem.at[step],
            recv_sem=recv_sem.at[step],
            device_id={"fs": fs_peer(step), "tp": me_tp},
            device_id_type=MESH_ID,
        )

    def send_tp(source, target, send_sem, recv_sem, step, target_tp):
        return pltpu.make_async_remote_copy(
            src_ref=source,
            dst_ref=target,
            send_sem=send_sem.at[step],
            recv_sem=recv_sem.at[step],
            device_id={"fs": me_fs, "tp": target_tp},
            device_id_type=MESH_ID,
        )

    def own_copy(source, target, slot):
        return pltpu.make_async_copy(source, target, load_sem.at[slot])

    loads = (
        own_copy(gate_hbm, gate_old, 2),
        own_copy(out_hbm, out_old, 3),
        own_copy(first_hbm, first_old, 4),
        own_copy(second_hbm, second_old, 5),
        own_copy(proj.at[0], all_proj.at[0, me_fs], 6),
        own_copy(proj.at[1], all_proj.at[1, me_fs], 7),
    )

    @pl.when(core == 0)
    def _():
        own_copy(tokens_in, left.at[0], 0).start()
        own_copy(gate_cot, right.at[0], 1).start()

    @pl.when(core == 1)
    def _():
        own_copy(block_cot, left.at[0], 0).start()
        own_copy(conv_out, right.at[0], 1).start()

    for load in loads:
        load.start()

    barrier = pltpu.get_barrier_semaphore()
    for step in range(1, fs_total):
        pl.semaphore_signal(
            barrier, inc=1, device_id={"fs": fs_peer(step), "tp": me_tp}, device_id_type=MESH_ID
        )
    for step in range(1, tp_total):
        pl.semaphore_signal(
            barrier, inc=1, device_id={"fs": me_fs, "tp": tp_peer(step)}, device_id_type=MESH_ID
        )
    pl.semaphore_wait(barrier, fs_total + tp_total - 2)

    proj_copies = [None]
    for step in range(1, fs_total):
        copy = send_fs(proj.at[core], all_proj.at[core, me_fs], proj_send, proj_recv, step)
        copy.start()
        proj_copies.append(copy)

    swap_left = send_tp(block_cot, left.at[1], swap_send, swap_recv, 0, partner)
    swap_right = send_tp(conv_out, right.at[1], swap_send, swap_recv, 1, partner)

    @pl.when(core == 0)
    def _():
        swap_left.start()
        swap_right.start()

    @pl.when(core == 1)
    def _():
        send_tp(tokens_in, left.at[1], swap_send, swap_recv, 0, partner).start()
        send_tp(gate_cot, right.at[1], swap_send, swap_recv, 1, partner).start()

    own_copy(tokens_in, left.at[0], 0).wait()
    swap_left.wait_recv()

    def mixed(block, factor_rows):
        columns = pl.ds(pl.multiple_of(block * rows_d, 128), rows_d)
        part = left[:, :, columns].reshape(2 * local, rows_d)
        return jnp.dot(part, factor_rows, preferred_element_type=WIDE)

    pass_copies = [None]
    mix[...] = mixed(me_fs, proj[core])
    for step in range(1, fs_total):
        proj_copies[step].wait_recv()
        source = fs_source(step)
        block = all_proj.at[core, source]
        copy = send_tp(block, block, pass_send, pass_recv, step, partner)
        copy.start()
        pass_copies.append(copy)
        mix[...] += mixed(source, all_proj[core, source])

    own_copy(gate_cot, right.at[0], 1).wait()
    swap_right.wait_recv()
    upper = mix[...].astype(SLIM)
    lower = (mix[...] - upper.astype(WIDE)).astype(SLIM)
    cots = right[...].reshape(2 * local, right.shape[2])
    dims = (((0,), (0,)), ((), ()))
    low[...] = lax.dot_general(upper, cots, dims, preferred_element_type=WIDE) + lax.dot_general(
        lower, cots, dims, preferred_element_type=WIDE
    )

    def low_rows(block):
        return low[pl.ds(pl.multiple_of(block * rank_rows, 8), rank_rows), :]

    fs_copies = [None]
    for step in range(1, fs_total):
        rows = low_rows(fs_peer(step)).astype(SLIM)
        for tile in range(tp_total):
            fs_out[step, tile] = rows[:, tile * width : (tile + 1) * width]
        copy = send_fs(fs_out.at[step], fs_in.at[step], fs_send, fs_recv, step)
        copy.start()
        fs_copies.append(copy)
    loads[0].wait()
    loads[1].wait()
    gate_slim[me_fs] = gate_old[...].astype(SLIM)
    out_slim[me_fs] = out_old[...].astype(SLIM)
    last_copies = []
    for step in range(1, fs_total):
        block = gate_slim.at[me_fs]
        copy = send_fs(block, block, gate_send, gate_recv, step)
        copy.start()
        last_copies.append(copy)
    rows = low_rows(me_fs)
    for tile in range(tp_total):
        tile_sum[tile] = rows[:, tile * width : (tile + 1) * width]
    for step in range(1, fs_total):
        fs_copies[step].wait_recv()
        tile_sum[...] += fs_in[step].astype(WIDE)

    tp_copies = [None]
    for step in range(1, tp_total):
        tp_out[step] = tile_sum[tp_peer(step)].astype(SLIM)
        copy = send_tp(tp_out.at[step], tp_in.at[step], tp_send, tp_recv, step, tp_peer(step))
        copy.start()
        tp_copies.append(copy)
    same = tile_sum[me_tp]
    other = None
    for step in range(1, tp_total):
        tp_copies[step].wait_recv()
        piece = tp_in[step].astype(WIDE)
        if step % 2 == 0:
            same = same + piece
        else:
            other = piece if other is None else other + piece

    loads[2].wait()
    loads[3].wait()
    lows = (jnp.where(core == 0, same, other), jnp.where(core == 0, other, same))
    for index in range(2):
        picked = pl.ds(index, rank_rows, stride=2)
        first = BETA_FIRST * first_old[picked, :] + (1.0 - BETA_FIRST) * lows[index]
        second = BETA_SECOND * second_old[picked, :] + (1.0 - BETA_SECOND) * lows[index] * lows[index]
        first_new[picked, :] = first
        second_new[picked, :] = second
        dirs[me_fs, index] = (first / jnp.sqrt(second)).astype(SLIM)

    dir_copies = [None]
    for step in range(1, fs_total):
        copy = send_fs(dirs.at[me_fs], dirs.at[me_fs], dir_send, dir_recv, step)
        copy.start()
        dir_copies.append(copy)
    for step in range(1, fs_total):
        block = out_slim.at[me_fs]
        copy = send_fs(block, block, out_send, out_recv, step)
        copy.start()
        last_copies.append(copy)
    for step in range(1, fs_total):
        dir_copies[step].wait_recv()

    gate_dir = dirs[:, 0].reshape(rank, width)
    flip_dir = dirs[:, 1].reshape(rank, width)
    gate_wide = gate_dir.astype(WIDE)
    flip_wide = flip_dir.astype(WIDE)
    squares[0, 0] = jnp.sum((gate_wide * gate_wide).reshape(rank // 8, 8, width), axis=0)
    squares[0, 1] = jnp.sum((flip_wide * flip_wide).reshape(rank // 8, 8, width), axis=0)
    square_copies = [None]
    for step in range(1, tp_total):
        copy = send_tp(
            squares.at[0], squares.at[step], square_send, square_recv, step, tp_peer(step)
        )
        copy.start()
        square_copies.append(copy)
    for step in range(1, tp_total):
        square_copies[step].wait()
        tp_copies[step].wait_send()
    for step in range(1, fs_total):
        proj_copies[step].wait_send()
        pass_copies[step].wait()
        fs_copies[step].wait_send()
        dir_copies[step].wait_send()
    loads[4].wait()
    loads[5].wait()
    swap_left.wait_send()
    swap_right.wait_send()
    for copy in last_copies:
        copy.wait()


def finish_kernel(
    clip_level,
    first_in,
    second_in,
    dirs,
    squares,
    all_proj,
    gate_slim,
    out_slim,
    gate_old,
    out_old,
    first_new,
    second_new,
    step_gate,
    step_out,
    gate_new,
    out_new,
    gate_copy,
    out_copy,
    gate_step,
    out_step,
    gate_fresh,
    out_fresh,
    gate_round,
    out_round,
    sems,
):
    me_fs = lax.axis_index("fs")
    fs_total, _, rank_rows, width = dirs.shape
    rank = fs_total * rank_rows
    rows_d = all_proj.shape[2]
    stores = []

    def store(source, target):
        copy = pltpu.make_async_copy(source, target, sems.at[len(stores)])
        copy.start()
        stores.append(copy)

    store(first_in, first_new)
    store(second_in, second_new)
    totals = jnp.sum(squares[...], axis=0)
    gate_norm = jnp.sqrt(jnp.sum(totals[0], keepdims=True))
    flip_norm = jnp.sqrt(jnp.sum(totals[1], keepdims=True))
    gate_factor = clip_level / jnp.maximum(gate_norm, clip_level)
    out_factor = clip_level / jnp.maximum(flip_norm, clip_level)
    gate_dir = dirs[:, 0].reshape(rank, width)
    flip_dir = dirs[:, 1].reshape(rank, width)

    def gate_rows(block):
        return gate_factor * jnp.dot(all_proj[0, block], gate_dir, preferred_element_type=WIDE)

    def out_columns(block):
        return out_factor * lax.dot_general(
            flip_dir, all_proj[1, block], (((0,), (1,)), ((), ())), preferred_element_type=WIDE
        )

    for block in range(fs_total):
        part = pl.ds(block * rows_d, rows_d)
        fresh = gate_slim[block].astype(WIDE) - LEARN_RATE * gate_rows(block)
        gate_round[part, :] = fresh.astype(SLIM)
    store(gate_round, gate_copy)
    for block in range(fs_total):
        part = pl.ds(block * rows_d, rows_d)
        fresh = out_slim[block].astype(WIDE) - LEARN_RATE * out_columns(block)
        out_round[:, part] = fresh.astype(SLIM)
    store(out_round, out_copy)
    scaled = gate_rows(me_fs)
    gate_step[...] = scaled
    store(gate_step, step_gate)
    gate_fresh[...] = gate_old[...] - LEARN_RATE * scaled
    store(gate_fresh, gate_new)
    scaled = out_columns(me_fs)
    out_step[...] = scaled
    store(out_step, step_out)
    out_fresh[...] = out_old[...] - LEARN_RATE * scaled
    store(out_fresh, out_new)
    for copy in stores:
        copy.wait()


def held(array):
    return pltpu.with_memory_space_constraint(array, pltpu.HBM)


def shards(
    tokens_in,
    gate_cotangent,
    conv_output,
    block_cotangent,
    projectors,
    first_moment,
    second_moment,
    gate_master,
    out_master,
):
    fs_total = lax.axis_size("fs")
    tp_total = lax.axis_size("tp")
    local, model = tokens_in.shape
    channels = gate_cotangent.shape[1]
    rows_d, _, rank = projectors.shape
    rank_rows, _, width = first_moment.shape
    clip_level = CLIP_SHARE * math.sqrt(rank * channels)
    proj = jnp.transpose(projectors, (1, 0, 2))
    flat = (2 * rank_rows, width)
    shape = jax.ShapeDtypeStruct
    whole = pl.BlockSpec(memory_space=pltpu.VMEM)
    away = pl.BlockSpec(memory_space=pltpu.HBM)
    fs_sems = pltpu.SemaphoreType.DMA((fs_total,))
    tp_sems = pltpu.SemaphoreType.DMA((tp_total,))
    two_sems = pltpu.SemaphoreType.DMA((2,))
    middle = pl.pallas_call(
        functools.partial(exchange_kernel, fs_total, tp_total),
        out_shape=(
            shape(flat, WIDE),
            shape(flat, WIDE),
            shape((fs_total, 2, rank_rows, width), SLIM),
            shape((tp_total, 2, 8, width), WIDE),
            shape((2, fs_total, rows_d, rank), SLIM),
            shape((fs_total, rows_d, width), SLIM),
            shape((fs_total, width, rows_d), SLIM),
            shape((rows_d, width), WIDE),
            shape((width, rows_d), WIDE),
        ),
        in_specs=[away] * 4 + [whole] + [away] * 4,
        out_specs=(whole,) * 9,
        scratch_shapes=[
            pltpu.VMEM((2, local, model), SLIM),
            pltpu.VMEM((2, local, channels), SLIM),
            pltpu.VMEM((2 * local, rank), WIDE),
            pltpu.VMEM((rank, channels), WIDE),
            pltpu.VMEM((fs_total, tp_total, rank_rows, width), SLIM),
            pltpu.VMEM((fs_total, tp_total, rank_rows, width), SLIM),
            pltpu.VMEM((tp_total, rank_rows, width), WIDE),
            pltpu.VMEM((tp_total, rank_rows, width), SLIM),
            pltpu.VMEM((tp_total, rank_rows, width), SLIM),
            pltpu.VMEM(flat, WIDE),
            pltpu.VMEM(flat, WIDE),
            two_sems,
            two_sems,
            pltpu.SemaphoreType.DMA((8,)),
        ]
        + [fs_sems] * 6
        + [tp_sems] * 2
        + [fs_sems] * 2
        + [tp_sems] * 2
        + [fs_sems] * 4,
        compiler_params=pltpu.CompilerParams(
            collective_id=0, has_side_effects=True, vmem_limit_bytes=30 * 1024 * 1024
        ),
    )(
        held(tokens_in),
        held(gate_cotangent),
        held(conv_output),
        held(block_cotangent),
        proj,
        held(first_moment.reshape(flat)),
        held(second_moment.reshape(flat)),
        held(gate_master),
        held(out_master),
    )
    results = pl.pallas_call(
        functools.partial(finish_kernel, clip_level),
        out_shape=(
            shape(flat, WIDE),
            shape(flat, WIDE),
            shape((rows_d, width), WIDE),
            shape((width, rows_d), WIDE),
            shape((rows_d, width), WIDE),
            shape((width, rows_d), WIDE),
            shape((model, width), SLIM),
            shape((width, model), SLIM),
        ),
        in_specs=[whole] * 9,
        out_specs=(away,) * 8,
        scratch_shapes=[
            pltpu.VMEM((rows_d, width), WIDE),
            pltpu.VMEM((width, rows_d), WIDE),
            pltpu.VMEM((rows_d, width), WIDE),
            pltpu.VMEM((width, rows_d), WIDE),
            pltpu.VMEM((model, width), SLIM),
            pltpu.VMEM((width, model), SLIM),
            pltpu.SemaphoreType.DMA((8,)),
        ],
        compiler_params=pltpu.CompilerParams(vmem_limit_bytes=30 * 1024 * 1024),
    )(*middle)
    first_new, second_new = (part.reshape(rank_rows, 2, width) for part in results[:2])
    return (first_new, second_new) + tuple(results[2:])


def solution(mesh):
    in_specs = (
        P(("fs", "tp"), None),
        P(("fs", "tp"), None),
        P(("fs", "tp"), None),
        P(("fs", "tp"), None),
        P("fs", None, None),
        P("fs", None, "tp"),
        P("fs", None, "tp"),
        P("fs", "tp"),
        P("tp", "fs"),
    )
    out_specs = (
        P("fs", None, "tp"),
        P("fs", None, "tp"),
        P("fs", "tp"),
        P("tp", "fs"),
        P("fs", "tp"),
        P("tp", "fs"),
        P(None, "tp"),
        P("tp", None),
    )
    return jax.shard_map(shards, mesh=mesh, in_specs=in_specs, out_specs=out_specs, check_vma=False)
```

```python
import functools
import math

import jax
import jax.numpy as jnp
from jax import lax
from jax.experimental import pallas as pl
from jax.experimental.pallas import tpu as pltpu
from jax.sharding import PartitionSpec as P

BETA_FIRST = 0.8
BETA_SECOND = 0.9
LEARN_RATE = 0.01
CLIP_SHARE = 0.5
MESH_ID = pl.DeviceIdType.MESH
WIDE = jnp.float32
SLIM = jnp.bfloat16


def exchange_kernel(
    fs_total,
    tp_total,
    tokens_in,
    gate_cot,
    conv_out,
    block_cot,
    proj,
    first_hbm,
    second_hbm,
    gate_hbm,
    out_hbm,
    first_new,
    second_new,
    dirs,
    squares,
    all_proj,
    gate_slim,
    out_slim,
    gate_old,
    out_old,
    left,
    right,
    mix,
    low,
    fs_out,
    fs_in,
    tile_sum,
    tp_out,
    tp_in,
    first_old,
    second_old,
    tp_squares,
    swap_send,
    swap_recv,
    load_sem,
    proj_send,
    proj_recv,
    pass_send,
    pass_recv,
    fs_send,
    fs_recv,
    tp_send,
    tp_recv,
    dir_send,
    dir_recv,
    square_send,
    square_recv,
    gate_send,
    gate_recv,
    out_send,
    out_recv,
    sum_send,
    sum_recv,
):
    me_fs = lax.axis_index("fs")
    me_tp = lax.axis_index("tp")
    core = lax.rem(me_tp, 2)
    partner = me_tp + 1 - 2 * core
    rows_d, rank = proj.shape[1], proj.shape[2]
    rank_rows = rank // fs_total
    width = gate_old.shape[1]
    local = tokens_in.shape[0]

    def fs_peer(step):
        return lax.rem(me_fs + step, fs_total)

    def fs_source(step):
        return lax.rem(me_fs + fs_total - step, fs_total)

    def tp_peer(step):
        return lax.rem(me_tp + step, tp_total)

    def send_fs(source, target, send_sem, recv_sem, step):
        return pltpu.make_async_remote_copy(
            src_ref=source,
            dst_ref=target,
            send_sem=send_sem.at[step],
            recv_sem=recv_sem.at[step],
            device_id={"fs": fs_peer(step), "tp": me_tp},
            device_id_type=MESH_ID,
        )

    def send_tp(source, target, send_sem, recv_sem, step, target_tp):
        return pltpu.make_async_remote_copy(
            src_ref=source,
            dst_ref=target,
            send_sem=send_sem.at[step],
            recv_sem=recv_sem.at[step],
            device_id={"fs": me_fs, "tp": target_tp},
            device_id_type=MESH_ID,
        )

    def own_copy(source, target, slot):
        return pltpu.make_async_copy(source, target, load_sem.at[slot])

    loads = (
        own_copy(gate_hbm, gate_old, 2),
        own_copy(out_hbm, out_old, 3),
        own_copy(first_hbm, first_old, 4),
        own_copy(second_hbm, second_old, 5),
        own_copy(proj.at[0], all_proj.at[0, me_fs], 6),
        own_copy(proj.at[1], all_proj.at[1, me_fs], 7),
    )

    @pl.when(core == 0)
    def _():
        own_copy(tokens_in, left.at[0], 0).start()
        own_copy(gate_cot, right.at[0], 1).start()

    @pl.when(core == 1)
    def _():
        own_copy(block_cot, left.at[0], 0).start()
        own_copy(conv_out, right.at[0], 1).start()

    for load in loads:
        load.start()

    barrier = pltpu.get_barrier_semaphore()
    for step in range(1, fs_total):
        pl.semaphore_signal(
            barrier, inc=1, device_id={"fs": fs_peer(step), "tp": me_tp}, device_id_type=MESH_ID
        )
    for step in range(1, tp_total):
        pl.semaphore_signal(
            barrier, inc=1, device_id={"fs": me_fs, "tp": tp_peer(step)}, device_id_type=MESH_ID
        )
    pl.semaphore_wait(barrier, fs_total + tp_total - 2)

    quad = fs_total == 4
    beside = me_fs + 1 - 2 * lax.rem(me_fs, 2)
    above = lax.rem(me_fs + 2, fs_total)
    half = rows_d // 2

    def send_half(target, owner, part, index):
        rows = pl.ds(part * half, half)
        block = all_proj.at[core, owner, rows]
        mine = owner is me_fs
        return pltpu.make_async_remote_copy(
            src_ref=proj.at[core, rows] if mine else block,
            dst_ref=block,
            send_sem=proj_send.at[index],
            recv_sem=proj_recv.at[index],
            device_id={"fs": target, "tp": me_tp},
            device_id_type=MESH_ID,
        )

    proj_copies = []
    if quad:
        plan = ((beside, 0), (above, 1), (beside, 1), (above, 0))
        for index, (target, part) in enumerate(plan):
            copy = send_half(target, me_fs, part, index)
            copy.start()
            proj_copies.append(copy)
    else:
        for step in range(1, fs_total):
            copy = send_fs(
                proj.at[core], all_proj.at[core, me_fs], proj_send, proj_recv, step
            )
            copy.start()
            proj_copies.append(copy)

    swap_left = send_tp(block_cot, left.at[1], swap_send, swap_recv, 0, partner)
    swap_right = send_tp(conv_out, right.at[1], swap_send, swap_recv, 1, partner)

    @pl.when(core == 0)
    def _():
        swap_left.start()
        swap_right.start()

    @pl.when(core == 1)
    def _():
        send_tp(tokens_in, left.at[1], swap_send, swap_recv, 0, partner).start()
        send_tp(gate_cot, right.at[1], swap_send, swap_recv, 1, partner).start()

    own_copy(tokens_in, left.at[0], 0).wait()
    swap_left.wait_recv()

    def mixed(block, factor_rows):
        columns = pl.ds(pl.multiple_of(block * rows_d, 128), rows_d)
        part = left[:, :, columns].reshape(2 * local, rows_d)
        return jnp.dot(part, factor_rows, preferred_element_type=WIDE)

    mix[...] = mixed(me_fs, proj[core])
    loads[0].wait()
    gate_slim[me_fs] = gate_old[...].astype(SLIM)
    last_copies = []
    pass_copies = []

    def send_gate():
        for step in range(1, fs_total):
            block = gate_slim.at[me_fs]
            copy = send_fs(block, block, gate_send, gate_recv, step)
            copy.start()
            last_copies.append(copy)

    def absorb(source):
        block = all_proj.at[core, source]
        step = len(pass_copies) + 1
        copy = send_tp(block, block, pass_send, pass_recv, step, partner)
        copy.start()
        pass_copies.append(copy)
        mix[...] += mixed(source, all_proj[core, source])

    if quad:
        for index, (target, owner, part) in enumerate(((above, beside, 0), (beside, above, 1))):
            proj_copies[index].wait_recv()
            copy = send_half(target, owner, part, index + 4)
            copy.start()
            proj_copies.append(copy)
        send_gate()
        proj_copies[2].wait_recv()
        absorb(beside)
        proj_copies[3].wait_recv()
        absorb(above)
        proj_copies[4].wait_recv()
        proj_copies[5].wait_recv()
        absorb(fs_total - 1 - me_fs)
    else:
        for step in range(1, fs_total):
            proj_copies[step - 1].wait_recv()
            if step == fs_total - 1:
                send_gate()
            absorb(fs_source(step))

    own_copy(gate_cot, right.at[0], 1).wait()
    swap_right.wait_recv()
    upper = mix[...].astype(SLIM)
    lower = (mix[...] - upper.astype(WIDE)).astype(SLIM)
    cots = right[...].reshape(2 * local, right.shape[2])
    dims = (((0,), (0,)), ((), ()))
    low[...] = lax.dot_general(upper, cots, dims, preferred_element_type=WIDE) + lax.dot_general(
        lower, cots, dims, preferred_element_type=WIDE
    )

    def low_rows(block):
        return low[pl.ds(pl.multiple_of(block * rank_rows, 8), rank_rows), :]

    fs_copies = [None]
    for step in range(1, fs_total):
        rows = low_rows(fs_peer(step)).astype(SLIM)
        for tile in range(tp_total):
            fs_out[step, tile] = rows[:, tile * width : (tile + 1) * width]
        copy = send_fs(fs_out.at[step], fs_in.at[step], fs_send, fs_recv, step)
        copy.start()
        fs_copies.append(copy)
    loads[1].wait()
    out_slim[me_fs] = out_old[...].astype(SLIM)
    for step in range(1, fs_total):
        block = out_slim.at[me_fs]
        copy = send_fs(block, block, out_send, out_recv, step)
        copy.start()
        last_copies.append(copy)
    rows = low_rows(me_fs)
    for tile in range(tp_total):
        tile_sum[tile] = rows[:, tile * width : (tile + 1) * width]
    for step in range(1, fs_total):
        fs_copies[step].wait_recv()
        tile_sum[...] += fs_in[step].astype(WIDE)

    tp_copies = [None]
    for step in range(1, tp_total):
        tp_out[step] = tile_sum[tp_peer(step)].astype(SLIM)
        copy = send_tp(tp_out.at[step], tp_in.at[step], tp_send, tp_recv, step, tp_peer(step))
        copy.start()
        tp_copies.append(copy)
    same = tile_sum[me_tp]
    other = None
    for step in range(1, tp_total):
        tp_copies[step].wait_recv()
        piece = tp_in[step].astype(WIDE)
        if step % 2 == 0:
            same = same + piece
        else:
            other = piece if other is None else other + piece

    loads[2].wait()
    loads[3].wait()
    lows = (jnp.where(core == 0, same, other), jnp.where(core == 0, other, same))
    for index in range(2):
        picked = pl.ds(index, rank_rows, stride=2)
        first = BETA_FIRST * first_old[picked, :] + (1.0 - BETA_FIRST) * lows[index]
        second = BETA_SECOND * second_old[picked, :] + (1.0 - BETA_SECOND) * lows[index] * lows[index]
        first_new[picked, :] = first
        second_new[picked, :] = second
        direction = first / jnp.sqrt(second)
        dirs[me_fs, index] = direction.astype(SLIM)
        tp_squares[0, index] = jnp.sum(
            (direction * direction).reshape(rank_rows // 8, 8, width), axis=0
        )

    dir_copies = [None]
    for step in range(1, fs_total):
        copy = send_fs(dirs.at[me_fs], dirs.at[me_fs], dir_send, dir_recv, step)
        copy.start()
        dir_copies.append(copy)
    square_copies = []
    for step in range(1, tp_total):
        copy = send_tp(
            tp_squares.at[0], tp_squares.at[step], square_send, square_recv, step, tp_peer(step)
        )
        copy.start()
        square_copies.append(copy)
    for copy in square_copies:
        copy.wait_recv()
    squares[me_fs] = jnp.sum(tp_squares[...], axis=0)
    sum_copies = []
    for step in range(1, fs_total):
        block = squares.at[me_fs]
        copy = send_fs(block, block, sum_send, sum_recv, step)
        copy.start()
        sum_copies.append(copy)
    for copy in square_copies + proj_copies:
        copy.wait_send()
    for copy in pass_copies + sum_copies:
        copy.wait()
    for step in range(1, tp_total):
        tp_copies[step].wait_send()
    for step in range(1, fs_total):
        fs_copies[step].wait_send()
        dir_copies[step].wait()
    loads[4].wait()
    loads[5].wait()
    swap_left.wait_send()
    swap_right.wait_send()
    for copy in last_copies:
        copy.wait()


def finish_kernel(
    clip_level,
    first_in,
    second_in,
    dirs,
    squares,
    all_proj,
    gate_slim,
    out_slim,
    gate_old,
    out_old,
    first_new,
    second_new,
    step_gate,
    step_out,
    gate_new,
    out_new,
    gate_copy,
    out_copy,
    gate_step,
    out_step,
    gate_fresh,
    out_fresh,
    gate_round,
    out_round,
    sems,
):
    me_fs = lax.axis_index("fs")
    fs_total, _, rank_rows, width = dirs.shape
    rank = fs_total * rank_rows
    rows_d = all_proj.shape[2]
    stores = []

    def store(source, target):
        copy = pltpu.make_async_copy(source, target, sems.at[len(stores)])
        copy.start()
        stores.append(copy)

    store(first_in, first_new)
    store(second_in, second_new)
    totals = jnp.sum(squares[...], axis=0)
    gate_norm = jnp.sqrt(jnp.sum(totals[0], keepdims=True))
    flip_norm = jnp.sqrt(jnp.sum(totals[1], keepdims=True))
    gate_factor = clip_level / jnp.maximum(gate_norm, clip_level)
    out_factor = clip_level / jnp.maximum(flip_norm, clip_level)
    gate_dir = dirs[:, 0].reshape(rank, width)
    flip_dir = dirs[:, 1].reshape(rank, width)

    def gate_rows(block):
        return gate_factor * jnp.dot(all_proj[0, block], gate_dir, preferred_element_type=WIDE)

    def out_columns(block):
        return out_factor * lax.dot_general(
            flip_dir, all_proj[1, block], (((0,), (1,)), ((), ())), preferred_element_type=WIDE
        )

    for block in range(fs_total):
        part = pl.ds(block * rows_d, rows_d)
        fresh = gate_slim[block].astype(WIDE) - LEARN_RATE * gate_rows(block)
        gate_round[part, :] = fresh.astype(SLIM)
    store(gate_round, gate_copy)
    for block in range(fs_total):
        part = pl.ds(block * rows_d, rows_d)
        fresh = out_slim[block].astype(WIDE) - LEARN_RATE * out_columns(block)
        out_round[:, part] = fresh.astype(SLIM)
    store(out_round, out_copy)
    scaled = gate_rows(me_fs)
    gate_step[...] = scaled
    store(gate_step, step_gate)
    gate_fresh[...] = gate_old[...] - LEARN_RATE * scaled
    store(gate_fresh, gate_new)
    scaled = out_columns(me_fs)
    out_step[...] = scaled
    store(out_step, step_out)
    out_fresh[...] = out_old[...] - LEARN_RATE * scaled
    store(out_fresh, out_new)
    for copy in stores:
        copy.wait()


def held(array):
    return pltpu.with_memory_space_constraint(array, pltpu.HBM)


def shards(
    tokens_in,
    gate_cotangent,
    conv_output,
    block_cotangent,
    projectors,
    first_moment,
    second_moment,
    gate_master,
    out_master,
):
    fs_total = lax.axis_size("fs")
    tp_total = lax.axis_size("tp")
    local, model = tokens_in.shape
    channels = gate_cotangent.shape[1]
    rows_d, _, rank = projectors.shape
    rank_rows, _, width = first_moment.shape
    clip_level = CLIP_SHARE * math.sqrt(rank * channels)
    proj = jnp.transpose(projectors, (1, 0, 2))
    flat = (2 * rank_rows, width)
    shape = jax.ShapeDtypeStruct
    whole = pl.BlockSpec(memory_space=pltpu.VMEM)
    away = pl.BlockSpec(memory_space=pltpu.HBM)
    fs_sems = pltpu.SemaphoreType.DMA((fs_total,))
    tp_sems = pltpu.SemaphoreType.DMA((tp_total,))
    two_sems = pltpu.SemaphoreType.DMA((2,))
    middle = pl.pallas_call(
        functools.partial(exchange_kernel, fs_total, tp_total),
        out_shape=(
            shape(flat, WIDE),
            shape(flat, WIDE),
            shape((fs_total, 2, rank_rows, width), SLIM),
            shape((fs_total, 2, 8, width), WIDE),
            shape((2, fs_total, rows_d, rank), SLIM),
            shape((fs_total, rows_d, width), SLIM),
            shape((fs_total, width, rows_d), SLIM),
            shape((rows_d, width), WIDE),
            shape((width, rows_d), WIDE),
        ),
        in_specs=[away] * 4 + [whole] + [away] * 4,
        out_specs=(whole,) * 9,
        scratch_shapes=[
            pltpu.VMEM((2, local, model), SLIM),
            pltpu.VMEM((2, local, channels), SLIM),
            pltpu.VMEM((2 * local, rank), WIDE),
            pltpu.VMEM((rank, channels), WIDE),
            pltpu.VMEM((fs_total, tp_total, rank_rows, width), SLIM),
            pltpu.VMEM((fs_total, tp_total, rank_rows, width), SLIM),
            pltpu.VMEM((tp_total, rank_rows, width), WIDE),
            pltpu.VMEM((tp_total, rank_rows, width), SLIM),
            pltpu.VMEM((tp_total, rank_rows, width), SLIM),
            pltpu.VMEM(flat, WIDE),
            pltpu.VMEM(flat, WIDE),
            pltpu.VMEM((tp_total, 2, 8, width), WIDE),
            two_sems,
            two_sems,
            pltpu.SemaphoreType.DMA((8,)),
        ]
        + [pltpu.SemaphoreType.DMA((fs_total + 2,))] * 2
        + [fs_sems] * 4
        + [tp_sems] * 2
        + [fs_sems] * 2
        + [tp_sems] * 2
        + [fs_sems] * 6,
        compiler_params=pltpu.CompilerParams(
            collective_id=0, has_side_effects=True, vmem_limit_bytes=30 * 1024 * 1024
        ),
    )(
        held(tokens_in),
        held(gate_cotangent),
        held(conv_output),
        held(block_cotangent),
        proj,
        held(first_moment.reshape(flat)),
        held(second_moment.reshape(flat)),
        held(gate_master),
        held(out_master),
    )
    results = pl.pallas_call(
        functools.partial(finish_kernel, clip_level),
        out_shape=(
            shape(flat, WIDE),
            shape(flat, WIDE),
            shape((rows_d, width), WIDE),
            shape((width, rows_d), WIDE),
            shape((rows_d, width), WIDE),
            shape((width, rows_d), WIDE),
            shape((model, width), SLIM),
            shape((width, model), SLIM),
        ),
        in_specs=[whole] * 9,
        out_specs=(away,) * 8,
        scratch_shapes=[
            pltpu.VMEM((rows_d, width), WIDE),
            pltpu.VMEM((width, rows_d), WIDE),
            pltpu.VMEM((rows_d, width), WIDE),
            pltpu.VMEM((width, rows_d), WIDE),
            pltpu.VMEM((model, width), SLIM),
            pltpu.VMEM((width, model), SLIM),
            pltpu.SemaphoreType.DMA((8,)),
        ],
        compiler_params=pltpu.CompilerParams(vmem_limit_bytes=30 * 1024 * 1024),
    )(*middle)
    first_new, second_new = (part.reshape(rank_rows, 2, width) for part in results[:2])
    return (first_new, second_new) + tuple(results[2:])


def solution(mesh):
    in_specs = (
        P(("fs", "tp"), None),
        P(("fs", "tp"), None),
        P(("fs", "tp"), None),
        P(("fs", "tp"), None),
        P("fs", None, None),
        P("fs", None, "tp"),
        P("fs", None, "tp"),
        P("fs", "tp"),
        P("tp", "fs"),
    )
    out_specs = (
        P("fs", None, "tp"),
        P("fs", None, "tp"),
        P("fs", "tp"),
        P("tp", "fs"),
        P("fs", "tp"),
        P("tp", "fs"),
        P(None, "tp"),
        P("tp", None),
    )
    return jax.shard_map(shards, mesh=mesh, in_specs=in_specs, out_specs=out_specs, check_vma=False)
```
